32 devices in a mesh: fs: 8 (over z, x), tp: 4 (over y, core).
Axes of the slice: x: 2, y: 2, z: 4, core: 2. Of those that a mesh axis runs over, the one named last changes fastest.
Arguments:
- later_input: bfloat16 [6144, 2048], P('fs', 'tp'), may hold values from -6 to 6
- earlier_input: bfloat16 [6144, 2048], P('fs', 'tp'), may hold values from -6 to 6
- cotangent: bfloat16 [6144, 2048], P('fs', 'tp'), may hold values from -6 to 6
- up_weight: bfloat16 [2048, 8192], P('fs', 'tp'), may hold values from -0.125 to 0.125
- down_weight: bfloat16 [8192, 2048], P('tp', 'fs'), may hold values from -0.0625 to 0.0625
- up_running: float32 [2048, 8192], P('fs', 'tp'), may hold values from -6 to 6
- down_running: float32 [2048, 8192], P('fs', 'tp'), may hold values from -6 to 6
Outputs:
- later_output: bfloat16 [6144, 2048], P('fs', 'tp')
- later_preact: bfloat16 [6144, 8192], P('fs', 'tp')
- earlier_grad: bfloat16 [6144, 2048], P('fs', 'tp')
- up_running_out: float32 [2048, 8192], P('fs', 'tp')
- down_running_out: float32 [2048, 8192], P('fs', 'tp')
The draws below stay inside these ranges and needn't reach their ends.
All inputs are finite; a program needn't handle non-finite values.
Results may differ from the reference program's by a relative error of at most 0.014.
Values may be sent and summed in bfloat16 or wider, within the bound.
A program may use at most 128 MiB of HBM per device.

```python
import jax
import jax.numpy as jnp
from jax import lax

D = 2048
FF = 8192
TOKENS = 6144
N_TP = 4


def with_spikes(values, own_key, source, target, blocks, factor):
    def block_of(axis_at):
        return (jnp.arange(values.shape[axis_at]) // (values.shape[axis_at] // blocks)).reshape((-1,) + (1,) * (values.ndim - 1 - axis_at))

    near = jax.random.permutation(own_key, blocks)[block_of(target)]
    far = (block_of(target) + blocks // 2) % blocks
    return jnp.where((block_of(source) == near) | (block_of(source) == far), factor * values, values)


def steps_of(rng, shape, pieces, least, top_value):
    factor_of, own = 1.0, jax.random.fold_in(rng, 6)
    for position, blocks in pieces:
        steps = jnp.exp(jax.random.uniform(jax.random.fold_in(own, position), (blocks,), jnp.float32, least / len(pieces), top_value / len(pieces)))
        factor_of = factor_of * jnp.repeat(steps, shape[position] // blocks).reshape([-1 if axis == position else 1 for axis in range(len(shape))])
    return factor_of


def scatter_about(key, dims, scale, bound, split=(), kind=jnp.bfloat16):
    result = scale * jax.random.normal(key, dims, jnp.float32)
    if split:
        result = result * steps_of(key, dims, split, -0.22, 0.18)
    return jnp.clip(result, -bound, bound).astype(kind)


def heavy_noise(own_key, dims, scale, reach, split, heavy, held_as=jnp.bfloat16):
    drawn = scale * jax.random.normal(own_key, dims, jnp.float32)
    if split:
        drawn = drawn * steps_of(own_key, dims, split, -0.22, 0.18)
    return jnp.clip(with_spikes(drawn, jax.random.fold_in(own_key, 3), *heavy), -reach, reach).astype(held_as)


def setup_inputs(seed: int = 0) -> dict:
    splits = jax.random.split(jax.random.key(seed), 8)
    return {
        "later_input": scatter_about(splits[0], (TOKENS, D), 1.0, 6.0, ((0, 8), (1, 4))),
        "earlier_input": scatter_about(splits[1], (TOKENS, D), 1.0, 6.0, ((0, 8), (1, 4))),
        "cotangent": heavy_noise(splits[2], (TOKENS, D), 1.0, 6.0, ((0, 8), (1, 4)), (0, 1, 8, 2.0)),
        "up_weight": scatter_about(splits[3], (D, FF), D ** -0.5, 0.125, ((0, 8), (1, 4))),
        "down_weight": scatter_about(splits[4], (FF, D), FF ** -0.5, 0.0625, ((0, 4), (1, 8))),
        "up_running": scatter_about(splits[5], (D, FF), 1.0, 6.0, ((0, 8), (1, 4)), jnp.float32),
        "down_running": scatter_about(splits[6], (D, FF), 1.0, 6.0, ((0, 8), (1, 4)), jnp.float32),
    }


def block_sum(left, right):
    rows = left.shape[0]
    width = left.shape[1] // N_TP
    left_blocks = left.reshape(rows, N_TP, width).transpose(1, 0, 2)
    right_blocks = right.reshape(N_TP, width, right.shape[1])

    def step(total, pair):
        part = jnp.dot(pair[0], pair[1], preferred_element_type=jnp.float32).astype(jnp.bfloat16)
        part = lax.optimization_barrier(part)
        return total + part.astype(jnp.float32), None

    start = jnp.zeros((rows, right.shape[1]), jnp.float32)
    total, _ = lax.scan(step, start, (left_blocks, right_blocks))
    return total.astype(jnp.bfloat16)


def reference(later_input, earlier_input, cotangent, up_weight, down_weight, up_running, down_running):
    later_up = jnp.dot(later_input, up_weight, preferred_element_type=jnp.float32)
    later_preact = later_up.astype(jnp.bfloat16)
    later_hidden = jnp.square(jax.nn.relu(later_up)).astype(jnp.bfloat16)
    later_output = block_sum(later_hidden, down_weight)
    earlier_up = jnp.dot(earlier_input, up_weight, preferred_element_type=jnp.float32)
    earlier_hidden = jnp.square(jax.nn.relu(earlier_up)).astype(jnp.bfloat16)
    hidden_grad = jnp.dot(cotangent, down_weight.T, preferred_element_type=jnp.float32)
    up_grad = (2.0 * jax.nn.relu(earlier_up) * hidden_grad).astype(jnp.bfloat16)
    earlier_grad = block_sum(up_grad, up_weight.T)
    factor = float(TOKENS) ** -0.5
    up_running_out = up_running + jnp.dot(earlier_input.T, up_grad, preferred_element_type=jnp.float32) * factor
    down_running_out = down_running + jnp.dot(cotangent.T, earlier_hidden, preferred_element_type=jnp.float32) * factor
    return later_output, later_preact, earlier_grad, up_running_out, down_running_out
```

```python
import jax
import jax.numpy as jnp
from jax import lax
from jax.sharding import PartitionSpec as P

contract_last = (((1,), (1,)), ((), ()))
contract_first = (((0,), (0,)), ((), ()))


STREAMS = 4


def ring_index(place, n):
    place = lax.rem(place + 2 * n, n)
    return jnp.where(place < n // 2, 2 * place, 2 * (n - place) - 1)


def ring_pairs(n, direction):
    order = [q * 2 if q < n // 2 else 2 * (n - q) - 1 for q in range(n)]
    return [(order[q], order[(q + direction) % n]) for q in range(n)]


def my_place(n):
    me = lax.axis_index("fs")
    half = lax.div(me, 2)
    return jnp.where(lax.rem(me, 2) == 0, half, n - 1 - half)


def after(value, *others):
    return lax.optimization_barrier((value, *others))[0]


def ring_gather(shard):
    n = lax.axis_size("fs")
    rows, columns = shard.shape
    place = my_place(n)
    blocks = shard.reshape(STREAMS, rows // STREAMS, columns)
    held = [blocks[s : s + 1] for s in range(STREAMS)]
    full = jnp.zeros((n, STREAMS, rows // STREAMS, columns), shard.dtype)
    full = lax.dynamic_update_slice(full, blocks[None], (lax.axis_index("fs"), 0, 0, 0))
    arrived = []
    for step in range(1, n):
        for s in range(STREAMS):
            direction = 1 if s % 2 == 0 else -1
            held[s] = lax.ppermute(held[s], "fs", ring_pairs(n, direction))
            owner = ring_index(place - direction * step, n)
            full = lax.dynamic_update_slice(full, held[s][None], (owner, s, 0, 0))
        arrived.append(tuple(held))
    return full.reshape(n * rows, columns), arrived


def ring_scatter(terms, wait_for=()):
    n = lax.axis_size("fs")
    rows, columns = terms.shape[0] // n, terms.shape[1]
    place = my_place(n)
    blocks = terms.reshape(n, STREAMS, rows // STREAMS, columns)

    def own(s, direction, step):
        owner = ring_index(place - direction * (step + 1), n)
        return lax.dynamic_slice(
            blocks, (owner, s, 0, 0), (1, 1, rows // STREAMS, columns)
        ).reshape(rows // STREAMS, columns)

    totals = [own(s, 1 if s % 2 == 0 else -1, 0) for s in range(STREAMS)]
    if wait_for:
        totals = [after(total, *wait_for) for total in totals]
    for step in range(1, n):
        for s in range(STREAMS):
            direction = 1 if s % 2 == 0 else -1
            got = lax.ppermute(
                totals[s].astype(jnp.bfloat16), "fs", ring_pairs(n, direction)
            )
            totals[s] = got.astype(jnp.float32) + own(s, direction, step).astype(jnp.float32)
    return jnp.concatenate(totals, axis=0)


def flip_pairs(n, mask):
    return [(i, i ^ mask) for i in range(n)]


def tp_gather(block):
    n = lax.axis_size("tp")
    me = lax.axis_index("tp")
    blocks = [block]
    mask = n // 2
    while mask:
        upper = (me & mask) != 0
        merged = []
        for mine in blocks:
            other = lax.ppermute(mine, "tp", flip_pairs(n, mask))
            merged += [jnp.where(upper, other, mine), jnp.where(upper, mine, other)]
        blocks = merged
        mask //= 2
    return jnp.concatenate(blocks, axis=-1)


def tp_scatter(terms):
    n = lax.axis_size("tp")
    me = lax.axis_index("tp")
    width = terms.shape[1] // n
    blocks = [terms[:, j * width : (j + 1) * width] for j in range(n)]
    mask = 1
    while mask < n:
        upper = (me & mask) != 0
        kept = []
        for low, high in zip(blocks[0::2], blocks[1::2]):
            sent = jnp.where(upper, low, high).astype(jnp.bfloat16)
            mine = jnp.where(upper, high, low)
            got = lax.ppermute(sent, "tp", flip_pairs(n, mask))
            kept.append(mine.astype(jnp.float32) + got.astype(jnp.float32))
        blocks = kept
        mask *= 2
    return blocks[0].astype(jnp.bfloat16)


def on_device(
    later_input, earlier_input, cotangent, up_weight, down_weight, up_running, down_running
):
    n = lax.axis_size("fs")
    factor = float(later_input.shape[0] * n) ** (-0.5)

    up_full, up_arrived = ring_gather(up_weight)
    inputs = tp_gather(jnp.stack((later_input, earlier_input, cotangent)))
    later_full, earlier_full, cot_full = inputs[0], inputs[1], inputs[2]
    down_rows = after(down_weight.T, inputs, *up_arrived[-2])
    down_full, down_arrived = ring_gather(down_rows)

    earlier_up = jnp.dot(earlier_full, up_full, preferred_element_type=jnp.float32)
    earlier_relu = jax.nn.relu(earlier_up)
    earlier_hidden = jnp.square(earlier_relu).astype(jnp.bfloat16)
    down_terms = lax.dot_general(
        cot_full, earlier_hidden, contract_first, preferred_element_type=jnp.float32
    ).astype(jnp.bfloat16)
    down_sum = ring_scatter(down_terms, down_arrived[-2])

    later_up = jnp.dot(later_full, up_full, preferred_element_type=jnp.float32)
    later_preact = later_up.astype(jnp.bfloat16)
    later_hidden = jnp.square(jax.nn.relu(later_up)).astype(jnp.bfloat16)

    grad = jnp.dot(cot_full, down_full, preferred_element_type=jnp.float32)
    up_grad = (2.0 * earlier_relu * grad).astype(jnp.bfloat16)
    up_terms = lax.dot_general(
        earlier_full, up_grad, contract_first, preferred_element_type=jnp.float32
    ).astype(jnp.bfloat16)
    up_sum = ring_scatter(up_terms)

    back_part = lax.dot_general(
        up_grad, up_full, contract_last, preferred_element_type=jnp.float32
    ).astype(jnp.bfloat16)
    product = lax.dot_general(
        later_hidden, down_full, contract_last, preferred_element_type=jnp.float32
    ).astype(jnp.bfloat16)
    return (
        tp_scatter(product),
        later_preact,
        tp_scatter(back_part),
        up_running + up_sum * factor,
        down_running + down_sum * factor,
    )


def solution(mesh):
    in_specs = (
        P("fs", "tp"),
        P("fs", "tp"),
        P("fs", "tp"),
        P("fs", "tp"),
        P("tp", "fs"),
        P("fs", "tp"),
        P("fs", "tp"),
    )
    out_specs = (P("fs", "tp"), P("fs", "tp"), P("fs", "tp"), P("fs", "tp"), P("fs", "tp"))
    return jax.shard_map(
        on_device, mesh=mesh, in_specs=in_specs, out_specs=out_specs, check_vma=False
    )
```

```python
import jax
import jax.numpy as jnp
from jax import lax
from jax.sharding import PartitionSpec as P

contract_last = (((1,), (1,)), ((), ()))
contract_first = (((0,), (0,)), ((), ()))


STREAMS = 4


def ring_index(place, n):
    place = lax.rem(place + 2 * n, n)
    return jnp.where(place < n // 2, 2 * place, 2 * (n - place) - 1)


def ring_pairs(n, direction):
    order = [q * 2 if q < n // 2 else 2 * (n - q) - 1 for q in range(n)]
    return [(order[q], order[(q + direction) % n]) for q in range(n)]


def my_place(n):
    me = lax.axis_index("fs")
    half = lax.div(me, 2)
    return jnp.where(lax.rem(me, 2) == 0, half, n - 1 - half)


def after(value, *others):
    return lax.optimization_barrier((value, *others))[0]


def ring_gather(shard):
    n = lax.axis_size("fs")
    rows, columns = shard.shape
    place = my_place(n)
    blocks = shard.reshape(STREAMS, rows // STREAMS, columns)
    held = [blocks[s : s + 1] for s in range(STREAMS)]
    full = jnp.zeros((n, STREAMS, rows // STREAMS, columns), shard.dtype)
    full = lax.dynamic_update_slice(full, blocks[None], (lax.axis_index("fs"), 0, 0, 0))
    arrived = []
    for step in range(1, n):
        for s in range(STREAMS):
            direction = 1 if s % 2 == 0 else -1
            held[s] = lax.ppermute(held[s], "fs", ring_pairs(n, direction))
            owner = ring_index(place - direction * step, n)
            full = lax.dynamic_update_slice(full, held[s][None], (owner, s, 0, 0))
        arrived.append(tuple(held))
    return full.reshape(n * rows, columns), arrived


def ring_scatter(terms, wait_for=()):
    n = lax.axis_size("fs")
    rows, columns = terms.shape[0] // n, terms.shape[1]
    place = my_place(n)
    blocks = terms.reshape(n, STREAMS, rows // STREAMS, columns)

    def own(s, direction, step):
        owner = ring_index(place - direction * (step + 1), n)
        return lax.dynamic_slice(
            blocks, (owner, s, 0, 0), (1, 1, rows // STREAMS, columns)
        ).reshape(rows // STREAMS, columns)

    totals = [own(s, 1 if s % 2 == 0 else -1, 0) for s in range(STREAMS)]
    if wait_for:
        totals = [after(total, *wait_for) for total in totals]
    for step in range(1, n):
        for s in range(STREAMS):
            direction = 1 if s % 2 == 0 else -1
            got = lax.ppermute(
                totals[s].astype(jnp.bfloat16), "fs", ring_pairs(n, direction)
            )
            totals[s] = got.astype(jnp.float32) + own(s, direction, step).astype(jnp.float32)
    return jnp.concatenate(totals, axis=0)


def flip_pairs(n, mask):
    return [(i, i ^ mask) for i in range(n)]


def tp_gather(block):
    n = lax.axis_size("tp")
    me = lax.axis_index("tp")
    blocks = [block]
    mask = n // 2
    while mask:
        upper = (me & mask) != 0
        merged = []
        for mine in blocks:
            other = lax.ppermute(mine, "tp", flip_pairs(n, mask))
            merged += [jnp.where(upper, other, mine), jnp.where(upper, mine, other)]
        blocks = merged
        mask //= 2
    return jnp.concatenate(blocks, axis=-1)


def tp_scatter(terms):
    n = lax.axis_size("tp")
    me = lax.axis_index("tp")
    width = terms.shape[1] // n
    blocks = [terms[:, j * width : (j + 1) * width] for j in range(n)]
    mask = 1
    while mask < n:
        upper = (me & mask) != 0
        kept = []
        for low, high in zip(blocks[0::2], blocks[1::2]):
            sent = jnp.where(upper, low, high).astype(jnp.bfloat16)
            mine = jnp.where(upper, high, low)
            got = lax.ppermute(sent, "tp", flip_pairs(n, mask))
            kept.append(mine.astype(jnp.float32) + got.astype(jnp.float32))
        blocks = kept
        mask *= 2
    return blocks[0].astype(jnp.bfloat16)


def on_device(
    later_input, earlier_input, cotangent, up_weight, down_weight, up_running, down_running
):
    n = lax.axis_size("fs")
    factor = float(later_input.shape[0] * n) ** (-0.5)

    up_full, up_arrived = ring_gather(up_weight)
    inputs = tp_gather(jnp.stack((later_input, earlier_input, cotangent)))
    later_full, earlier_full, cot_full = inputs[0], inputs[1], inputs[2]
    down_rows = after(down_weight.T, inputs, *up_arrived[-4])
    down_full, down_arrived = ring_gather(down_rows)

    earlier_up = jnp.dot(earlier_full, up_full, preferred_element_type=jnp.float32)
    earlier_relu = jax.nn.relu(earlier_up)
    earlier_hidden = jnp.square(earlier_relu).astype(jnp.bfloat16)
    down_terms = lax.dot_general(
        cot_full, earlier_hidden, contract_first, preferred_element_type=jnp.float32
    ).astype(jnp.bfloat16)
    down_sum = ring_scatter(down_terms, down_arrived[-4])

    later_up = jnp.dot(later_full, up_full, preferred_element_type=jnp.float32)
    later_preact = later_up.astype(jnp.bfloat16)
    later_hidden = jnp.square(jax.nn.relu(later_up)).astype(jnp.bfloat16)

    grad = jnp.dot(cot_full, down_full, preferred_element_type=jnp.float32)
    up_grad = (2.0 * earlier_relu * grad).astype(jnp.bfloat16)
    up_terms = lax.dot_general(
        earlier_full, up_grad, contract_first, preferred_element_type=jnp.float32
    ).astype(jnp.bfloat16)
    up_sum = ring_scatter(up_terms)

    back_part = lax.dot_general(
        up_grad, up_full, contract_last, preferred_element_type=jnp.float32
    ).astype(jnp.bfloat16)
    product = lax.dot_general(
        later_hidden, down_full, contract_last, preferred_element_type=jnp.float32
    ).astype(jnp.bfloat16)
    return (
        tp_scatter(product),
        later_preact,
        tp_scatter(back_part),
        up_running + up_sum * factor,
        down_running + down_sum * factor,
    )


def solution(mesh):
    in_specs = (
        P("fs", "tp"),
        P("fs", "tp"),
        P("fs", "tp"),
        P("fs", "tp"),
        P("tp", "fs"),
        P("fs", "tp"),
        P("fs", "tp"),
    )
    out_specs = (P("fs", "tp"), P("fs", "tp"), P("fs", "tp"), P("fs", "tp"), P("fs", "tp"))
    return jax.shard_map(
        on_device, mesh=mesh, in_specs=in_specs, out_specs=out_specs, check_vma=False
    )
```
